32 devices in a mesh: sp: 8 (over z, x), tp: 4 (over y, core).
Axes of the slice: x: 2, y: 2, z: 4, core: 2. Of those that a mesh axis runs over, the one named last changes fastest.
Arguments:
- residual: bfloat16 [4096, 2048], P('sp', 'tp'), may hold values from -64 to 64
- gains: float32 [2, 2, 2048], replicated, may hold values from 0.1 to 1.9
- w_query: bfloat16 [2, 2048, 2048], P(None, None, 'tp'), may hold values from -0.125 to 0.125
- w_key: bfloat16 [2, 2048, 2048], P(None, None, 'tp'), may hold values from -0.125 to 0.125
- w_value: bfloat16 [2, 2048, 2048], P(None, None, 'tp'), may hold values from -0.125 to 0.125
- w_out: bfloat16 [2, 2048, 2048], P(None, None, 'tp'), may hold values from -1 to 1
- rel_bias: float32 [2, 32, 257], P(None, 'tp'), may hold values from -6 to 300
Outputs:
- encoded: bfloat16 [4096, 2048], P('sp', 'tp')
The draws below stay inside these ranges and needn't reach their ends.
All inputs are finite; a program needn't handle non-finite values.
Results may differ from the reference program's by a relative error of at most 0.0058.
Values may be sent and summed in bfloat16 or wider, within the bound.
A program may use at most 128 MiB of HBM per device.

```python
import jax
import jax.numpy as jnp
from jax import lax

D = 2048
HEADS = 32
HEAD = 64
SEG = 64
LEFT = 8
MAXREL = 128
NREL = 257
LAYERS = 2
TOKENS = 4096


def rough_columns(key, col_count, rise_top):
    spread = jax.random.uniform(key, (col_count,), jnp.float32, -1.0, 1.0)
    ramp = jnp.arange(col_count, dtype=jnp.float32) / col_count
    return rise_top ** ramp * 2.0 ** spread


def draw_residual(key, part):
    key_base, key_rows, key_cols = jax.random.split(jax.random.fold_in(key, 11), 3)
    base = jnp.clip(jax.random.normal(key_base, (TOKENS, D), jnp.float32), -5.0, 5.0)
    row_scale = 0.3 * 10.0 ** jax.random.uniform(key_rows, (TOKENS, 1), jnp.float32)
    col_scale = rough_columns(key_cols, D, 3.0)
    return jnp.clip(base * row_scale * col_scale, -64.0, 64.0).astype(jnp.bfloat16)


def draw_w_out(key, part):
    key_base, key_cols = jax.random.split(jax.random.fold_in(key, 23), 2)
    base = jnp.clip(jax.random.normal(key_base, (LAYERS, D, D), jnp.float32), -5.0, 5.0)
    col_scale = rough_columns(key_cols, D, 3.0)
    scaled = base * col_scale / jnp.sqrt(jnp.float32(D))
    return jnp.clip(scaled, -1.0, 1.0).astype(jnp.bfloat16)


def draw_rel_bias(key, part):
    key_base = jax.random.fold_in(jax.random.fold_in(key, 37), 0)
    base = jnp.clip(jax.random.normal(key_base, (LAYERS, HEADS, NREL), jnp.float32), -6.0, 6.0)
    return base


def block_levels(stream_key, shape, shards, low, largest):
    loudness = 1.0
    for position, parts in shards:
        draws = jax.random.uniform(jax.random.fold_in(jax.random.fold_in(stream_key, 6), position), (parts,), jnp.float32, low / len(shards), largest / len(shards))
        loudness = loudness * jnp.repeat(jnp.exp(draws), shape[position] // parts).reshape((-1,) + (1,) * (len(shape) - 1 - position))
    return loudness


def gaussian(key, dims, scale, most, cuts=(), kind=jnp.bfloat16):
    factor_of = block_levels(key, dims, cuts, -0.22, 0.18) if cuts else 1.0
    values = jax.random.normal(key, dims, jnp.float32) * scale * factor_of
    return jnp.minimum(jnp.maximum(values, -most), most).astype(kind)


def setup_inputs(seed: int = 0) -> dict:
    keys = jax.random.split(jax.random.key(seed), 8)
    return {
        "residual": draw_residual(jax.random.fold_in(keys[7], 71), 0),
        "gains": jnp.clip(1.0 + 0.18 * jax.random.normal(keys[1], (LAYERS, 2, D), jnp.float32), 0.1, 1.9),
        "w_query": gaussian(keys[2], (LAYERS, D, D), D ** -0.5, 0.125, ((2, 4),)),
        "w_key": gaussian(keys[3], (LAYERS, D, D), D ** -0.5, 0.125, ((2, 4),)),
        "w_value": gaussian(keys[4], (LAYERS, D, D), D ** -0.5, 0.125, ((2, 4),)),
        "w_out": draw_w_out(jax.random.fold_in(keys[7], 71), 0),
        "rel_bias": draw_rel_bias(jax.random.fold_in(keys[7], 71), 0),
    }


norm_eps = 1e-06

def norm_rows(values, gain):
    widened = values.astype(jnp.float32)
    inv_rms = lax.rsqrt(lax.optimization_barrier(jnp.mean(widened * widened, axis=1, keepdims=True)) + norm_eps)
    return widened * inv_rms * gain

def attend_all(queries, key_rows, value_rows, bias_table):
    reach_rows = LEFT * SEG
    key_span = reach_rows + 128
    sub_count = queries.shape[0] // 128
    padding = jnp.zeros((reach_rows, key_rows.shape[1]), jnp.bfloat16)
    key_pad = jnp.concatenate([padding, key_rows], axis=0)
    value_pad = jnp.concatenate([padding, value_rows], axis=0)
    row_idx = jnp.arange(128, dtype=jnp.int32)[:, None]
    col_idx = jnp.arange(key_span, dtype=jnp.int32)[None, :]
    distance = reach_rows + row_idx - col_idx
    table_idx = jnp.clip(distance, -MAXREL, MAXREL) + MAXREL
    rel_terms = jnp.take(bias_table, table_idx, axis=1)

    def one_block(block_idx):
        start_row = (block_idx * 128).astype(jnp.int32)
        query_sub = lax.dynamic_slice_in_dim(queries, start_row, 128, 0).reshape(128, HEADS, HEAD).astype(jnp.float32)
        key_sub = lax.dynamic_slice_in_dim(key_pad, start_row, key_span, 0).reshape(key_span, HEADS, HEAD).astype(jnp.float32)
        value_sub = lax.dynamic_slice_in_dim(value_pad, start_row, key_span, 0).reshape(key_span, HEADS, HEAD).astype(jnp.float32)
        scores = jnp.einsum('qhd,khd->hqk', query_sub, key_sub) * HEAD ** (-0.5) + rel_terms
        query_pos = start_row + row_idx
        key_pos = start_row - reach_rows + col_idx
        seg_gap = jnp.floor_divide(query_pos, SEG) - jnp.floor_divide(key_pos, SEG)
        allowed = (key_pos >= 0) & (seg_gap >= 0) & (seg_gap <= LEFT)
        scores = jnp.where(allowed[None], scores, -jnp.inf)
        row_max = lax.optimization_barrier(jnp.max(scores, axis=2, keepdims=True))
        weights_raw = jnp.exp(scores - row_max)
        prob_bf = (weights_raw / lax.optimization_barrier(jnp.sum(weights_raw, axis=2, keepdims=True))).astype(jnp.bfloat16)
        result = jnp.einsum('hqk,khd->qhd', prob_bf.astype(jnp.float32), value_sub)
        return result.astype(jnp.bfloat16).reshape(128, HEADS * HEAD)
    blocks = lax.map(one_block, jnp.arange(sub_count, dtype=jnp.int32))
    return blocks.reshape(queries.shape[0], HEADS * HEAD)

def reference(residual, gains, w_query, w_key, w_value, w_out, rel_bias):
    stream = residual
    for layer_idx in range(LAYERS):
        normed = norm_rows(stream, gains[layer_idx, 0]).astype(jnp.bfloat16)
        queries = jnp.dot(normed, w_query[layer_idx], preferred_element_type=jnp.float32).astype(jnp.bfloat16)
        key_rows = jnp.dot(normed, w_key[layer_idx], preferred_element_type=jnp.float32).astype(jnp.bfloat16)
        value_rows = jnp.dot(normed, w_value[layer_idx], preferred_element_type=jnp.float32).astype(jnp.bfloat16)
        attended = attend_all(queries, key_rows, value_rows, rel_bias[layer_idx])
        branch = jnp.dot(attended, w_out[layer_idx], preferred_element_type=jnp.float32)
        stream = (stream.astype(jnp.float32) + norm_rows(branch, gains[layer_idx, 1])).astype(jnp.bfloat16)
    return stream
```

```python
import functools

import jax
import jax.numpy as jnp
from jax import lax
from jax.experimental import pallas as pl
from jax.experimental.pallas import tpu as pltpu
from jax.sharding import PartitionSpec as P

HEAD = 64
SEG = 64
LEFT = 8
MAXREL = 128
BLOCK = 128
EPS = 1e-06
LOG2E = 1.4426950408889634
NEG = -1e30
MESH = pl.DeviceIdType.MESH
F32 = jnp.float32
BF16 = jnp.bfloat16


def remote(src, dst, send_sem, recv_sem, where):
    return pltpu.make_async_remote_copy(
        src_ref=src,
        dst_ref=dst,
        send_sem=send_sem,
        recv_sem=recv_sem,
        device_id=where,
        device_id_type=MESH,
    )


def kernel(
    tp,
    sp_count,
    res_ref,
    gains_ref,
    bias_ref,
    wq_ref,
    wk_ref,
    wv_ref,
    wo_ref,
    out_ref,
    wbuf,
    gather,
    kbuf,
    vbuf,
    qbuf,
    branch,
    toeplitz,
    sums,
    w_sem,
    g_send,
    g_recv,
    f_send,
    h_send,
    h_recv,
    s_send,
    s_recv,
):
    layers = wbuf.shape[0]
    tokens, cols = res_ref.shape
    width = cols * tp
    chunks = tokens // BLOCK
    pairs = cols // 128
    reach = LEFT * SEG
    blocks = reach // BLOCK
    me = lax.axis_index("tp")
    sp = lax.axis_index("sp")
    core = lax.rem(me, 2)
    sibling = me + 1 - 2 * core
    ychips = tp // 2

    weights = (wq_ref, wk_ref, wv_ref, wo_ref)

    def weight_copy(l, k):
        return pltpu.make_async_copy(weights[k].at[l], wbuf.at[l, k], w_sem.at[l, k])

    for l in range(layers):
        for k in range(4):
            weight_copy(l, k).start()

    barrier = pltpu.get_barrier_semaphore()
    for k in range(1, tp):
        pl.semaphore_signal(
            barrier, inc=1, device_id={"tp": lax.rem(me + k, tp)}, device_id_type=MESH
        )
    for k in (1, sp_count - 1):
        pl.semaphore_signal(
            barrier, inc=1, device_id={"sp": lax.rem(sp + k, sp_count)}, device_id_type=MESH
        )
    pl.semaphore_wait(barrier, tp + 1)

    def rows_of(c):
        return pl.ds(pl.multiple_of(c * BLOCK, BLOCK), BLOCK)

    def block_of(kind, l, c, slot):
        return gather.at[kind, l, slot, rows_of(c)]

    def direct(kind, l, c, peer, source):
        ref = block_of(kind, l, c, source)
        return remote(
            ref, ref, g_send.at[kind, c, peer], g_recv.at[kind, l, c, source], {"tp": peer}
        )

    def forward(kind, l, c, source):
        ref = block_of(kind, l, c, source)
        return remote(
            ref, ref, f_send.at[source], g_recv.at[kind, l, c, source], {"tp": sibling}
        )

    def spread(kind, l, c):
        for k in range(1, ychips):
            direct(kind, l, c, lax.rem(me + 2 * k, tp), me).start()
        direct(kind, l, c, sibling, me).start()

    def arrive(kind, l, c):
        for k in range(1, ychips):
            source = lax.rem(me + 2 * k, tp)
            direct(kind, l, c, source, source).wait_recv()
            forward(kind, l, c, source).start()
        direct(kind, l, c, sibling, sibling).wait_recv()
        for k in range(1, ychips):
            source = lax.rem(sibling + 2 * k, tp)
            direct(kind, l, c, sibling, source).wait_recv()
        for k in range(1, ychips):
            forward(kind, l, c, lax.rem(me + 2 * k, tp)).wait_send()
            direct(kind, l, c, lax.rem(me + 2 * k, tp), me).wait_send()
        direct(kind, l, c, sibling, me).wait_send()

    def halo(l, c, which):
        buf = (kbuf, vbuf)[which]
        return remote(
            buf.at[l, rows_of(c + blocks)],
            buf.at[l, rows_of(c)],
            h_send.at[c, which],
            h_recv.at[l, c, which],
            {"sp": lax.rem(sp + 1, sp_count)},
        )

    def sum_copy(l, c, peer, source):
        ref = sums.at[l, c, source]
        return remote(ref, ref, s_send.at[peer], s_recv.at[l, c, source], {"tp": peer})

    gather[0, 0, me] = res_ref[...]
    for t in range(chunks):
        spread(0, 0, chunks - 1 - t)

    @pl.when(sp == 0)
    def _():
        for l in range(layers):
            kbuf[l, :reach] = jnp.zeros((reach, cols), BF16)
            vbuf[l, :reach] = jnp.zeros((reach, cols), BF16)

    row = lax.broadcasted_iota(jnp.int32, (BLOCK, BLOCK), 0)
    col = lax.broadcasted_iota(jnp.int32, (BLOCK, BLOCK), 1)
    low = col < HEAD
    early = jnp.where((row >= SEG) & (col < SEG), NEG, 0.0).astype(F32)
    late = jnp.where((row < SEG) & (col >= SEG), NEG, 0.0).astype(F32)

    def project(l, c):
        arrive(0, l, c)
        parts = [gather[0, l, j, rows_of(c)].astype(F32) for j in range(tp)]
        total = sum(jnp.sum(p * p, axis=1, keepdims=True) for p in parts)
        inv = lax.rsqrt(total / width + EPS)
        gain = gains_ref[l, 0:1, :]
        normed = jnp.concatenate(
            [
                (p * inv * gain[:, j * cols : (j + 1) * cols]).astype(BF16)
                for j, p in enumerate(parts)
            ],
            axis=1,
        )
        own = rows_of(c + blocks)
        kbuf[l, own] = jnp.dot(normed, wbuf[l, 1], preferred_element_type=F32).astype(BF16)
        vbuf[l, own] = jnp.dot(normed, wbuf[l, 2], preferred_element_type=F32).astype(BF16)

        @pl.when(sp < sp_count - 1)
        def _():
            halo(l, c, 0).start()
            halo(l, c, 1).start()

        query = jnp.dot(normed, wbuf[l, 0], preferred_element_type=F32)
        qbuf[rows_of(c)] = (query * (LOG2E * HEAD**-0.5)).astype(BF16)

    def attention(l, c):
        @pl.when(sp > 0)
        def _():
            halo(l, c, 0).wait_recv()
            halo(l, c, 1).wait_recv()

        @pl.when(sp < sp_count - 1)
        def _():
            halo(l, c, 0).wait_send()
            halo(l, c, 1).wait_send()

        window = pl.ds(pl.multiple_of(c * BLOCK, BLOCK), reach + BLOCK)
        closed = [
            jnp.where((sp == 0) & (c + i < blocks), NEG, 0.0).astype(F32) for i in range(blocks)
        ]

        for pair in range(pairs):
            lanes = slice(pair * 128, (pair + 1) * 128)
            query = qbuf[rows_of(c), lanes]
            keys = kbuf[l, window, lanes]
            values = vbuf[l, window, lanes]
            halves = []
            for half in range(2):
                mine = low if half == 0 else ~low
                masked = jnp.where(mine, query.astype(F32), 0.0).astype(BF16)
                scores = lax.dot_general(
                    masked, keys, (((1,), (1,)), ((), ())), preferred_element_type=F32
                )
                tiles = []
                for i in range(blocks + 1):
                    tile = scores[:, i * BLOCK : (i + 1) * BLOCK]
                    if i == 0:
                        tile = tile + early
                    if i >= blocks - 1:
                        at = (i - blocks + 1) * BLOCK
                        tile = tile + toeplitz[2 * pair + half, :, at : at + BLOCK]
                    if i < blocks:
                        tile = tile + closed[i]
                    tiles.append(tile)
                top = functools.reduce(jnp.maximum, tiles)
                top = jnp.max(top, axis=1, keepdims=True)
                tiles = [jnp.exp2(tile - top) for tile in tiles]
                total = jnp.sum(functools.reduce(jnp.add, tiles), axis=1, keepdims=True)
                raw = jnp.concatenate([tile.astype(BF16) for tile in tiles], axis=1)
                mixed = jnp.dot(raw, values, preferred_element_type=F32)
                halves.append(mixed / total)
            gather[1, l, me, rows_of(c), lanes] = jnp.where(low, halves[0], halves[1]).astype(BF16)
        spread(1, l, c)

    def out_project(l, c):
        arrive(1, l, c)
        whole = jnp.concatenate([gather[1, l, j, rows_of(c)] for j in range(tp)], axis=1)
        value = jnp.dot(whole, wbuf[l, 3], preferred_element_type=F32)
        branch[rows_of(c)] = value
        square = jnp.sum(value * value, axis=1, keepdims=True)
        sums[l, c, me] = jnp.broadcast_to(square, (BLOCK, BLOCK)).T[:8]
        for k in range(1, tp):
            sum_copy(l, c, lax.rem(me + k, tp), me).start()

    def finish(l, c):
        for k in range(1, tp):
            peer = lax.rem(me + k, tp)
            sum_copy(l, c, peer, peer).wait_recv()
            sum_copy(l, c, peer, me).wait_send()
        total = functools.reduce(jnp.add, [sums[l, c, j] for j in range(tp)])
        inv = lax.rsqrt(total / width + EPS)
        inv = jnp.broadcast_to(inv[0:1], (BLOCK, BLOCK)).T[:, 0:1]
        gain = gains_ref[l, 1:2, pl.ds(pl.multiple_of(me * cols, 128), cols)]
        new = gather[0, l, me, rows_of(c)].astype(F32) + branch[rows_of(c)] * inv * gain
        new = new.astype(BF16)

        @pl.when(l == layers - 1)
        def _():
            out_ref[rows_of(c)] = new

        @pl.when(l < layers - 1)
        def _():
            later = jnp.minimum(l + 1, layers - 1)
            gather[0, later, me, rows_of(c)] = new
            spread(0, later, c)

    def layer(l, carry):
        for h in range(2 * pairs):
            line = jnp.broadcast_to(bias_ref[l, h : h + 1], (BLOCK, bias_ref.shape[2]))
            skewed = pltpu.roll(line, 0, 1, stride=1, stride_axis=0)
            toeplitz[h, :, :BLOCK] = skewed[:, :BLOCK]
            toeplitz[h, :, BLOCK:] = skewed[:, BLOCK : 2 * BLOCK] + late
        for k in range(3):
            weight_copy(l, k).wait()

        def first(t, carry):
            project(l, chunks - 1 - t)
            return carry

        lax.fori_loop(0, chunks, first, 0)
        weight_copy(l, 3).wait()

        def second(t, carry):
            @pl.when(t < chunks)
            def _():
                attention(l, chunks - 1 - t)

            @pl.when((t >= 1) & (t <= chunks))
            def _():
                out_project(l, chunks - t)

            @pl.when(t >= 2)
            def _():
                finish(l, chunks + 1 - t)

            return carry

        lax.fori_loop(0, chunks + 2, second, 0)
        return carry

    lax.fori_loop(0, layers, layer, 0)


def on_device(tp, sp_count, residual, gains, w_query, w_key, w_value, w_out, rel_bias):
    tokens, cols = residual.shape
    layers, width, _ = w_query.shape
    chunks = tokens // BLOCK
    reach = LEFT * SEG
    heads = cols // HEAD
    far = rel_bias[:, :, 2 * MAXREL :]
    near = (rel_bias[:, :, 1:] - far)[:, :, ::-1] * LOG2E
    line = jnp.concatenate([near, jnp.zeros((layers, heads, BLOCK), F32)], axis=2)
    vmem = pl.BlockSpec(memory_space=pltpu.VMEM)
    hbm = pl.BlockSpec(memory_space=pl.ANY)
    dma = pltpu.SemaphoreType.DMA
    return pl.pallas_call(
        functools.partial(kernel, tp, sp_count),
        out_shape=jax.ShapeDtypeStruct((tokens, cols), BF16),
        in_specs=[vmem, vmem, vmem, hbm, hbm, hbm, hbm],
        out_specs=vmem,
        scratch_shapes=[
            pltpu.VMEM((layers, 4, width, cols), BF16),
            pltpu.VMEM((2, layers, tp, tokens, cols), BF16),
            pltpu.VMEM((layers, reach + tokens, cols), BF16),
            pltpu.VMEM((layers, reach + tokens, cols), BF16),
            pltpu.VMEM((tokens, cols), BF16),
            pltpu.VMEM((tokens, cols), F32),
            pltpu.VMEM((heads, BLOCK, 2 * BLOCK), F32),
            pltpu.VMEM((layers, chunks, tp, 8, BLOCK), F32),
            dma((layers, 4)),
            dma((2, chunks, tp)),
            dma((2, layers, chunks, tp)),
            dma((tp,)),
            dma((chunks, 2)),
            dma((layers, chunks, 2)),
            dma((tp,)),
            dma((layers, chunks, tp)),
        ],
        compiler_params=pltpu.CompilerParams(
            collective_id=0, has_side_effects=True, vmem_limit_bytes=58 * 2**20
        ),
    )(residual, gains, line, w_query, w_key, w_value, w_out)


def solution(mesh):
    return jax.shard_map(
        functools.partial(on_device, mesh.shape["tp"], mesh.shape["sp"]),
        mesh=mesh,
        in_specs=(
            P("sp", "tp"),
            P(),
            P(None, None, "tp"),
            P(None, None, "tp"),
            P(None, None, "tp"),
            P(None, None, "tp"),
            P(None, "tp", None),
        ),
        out_specs=P("sp", "tp"),
        check_vma=False,
    )
```

```python
import functools

import jax
import jax.numpy as jnp
from jax import lax
from jax.experimental import pallas as pl
from jax.experimental.pallas import tpu as pltpu
from jax.sharding import PartitionSpec as P

HEAD = 64
SEG = 64
LEFT = 8
MAXREL = 128
BLOCK = 128
EPS = 1e-06
LOG2E = 1.4426950408889634
NEG = -1e30
MESH = pl.DeviceIdType.MESH
F32 = jnp.float32
BF16 = jnp.bfloat16


def remote(src, dst, send_sem, recv_sem, where):
    return pltpu.make_async_remote_copy(
        src_ref=src,
        dst_ref=dst,
        send_sem=send_sem,
        recv_sem=recv_sem,
        device_id=where,
        device_id_type=MESH,
    )


def kernel(
    tp,
    sp_count,
    res_ref,
    gains_ref,
    bias_ref,
    wq_ref,
    wk_ref,
    wv_ref,
    wo_ref,
    out_ref,
    wbuf,
    gather,
    kbuf,
    vbuf,
    qbuf,
    branch,
    toeplitz,
    sums,
    w_sem,
    g_send,
    g_recv,
    f_send,
    h_send,
    h_recv,
    s_send,
    s_recv,
):
    layers = wbuf.shape[0]
    tokens, cols = res_ref.shape
    width = cols * tp
    chunks = tokens // BLOCK
    pairs = cols // 128
    reach = LEFT * SEG
    blocks = reach // BLOCK
    me = lax.axis_index("tp")
    sp = lax.axis_index("sp")
    core = lax.rem(me, 2)
    sibling = me + 1 - 2 * core
    ychips = tp // 2

    weights = (wq_ref, wk_ref, wv_ref, wo_ref)

    def weight_copy(l, k):
        return pltpu.make_async_copy(weights[k].at[l], wbuf.at[l, k], w_sem.at[l, k])

    for l in range(layers):
        for k in range(4):
            weight_copy(l, k).start()

    barrier = pltpu.get_barrier_semaphore()
    for k in range(1, tp):
        pl.semaphore_signal(
            barrier, inc=1, device_id={"tp": lax.rem(me + k, tp)}, device_id_type=MESH
        )
    for k in (1, sp_count - 1):
        pl.semaphore_signal(
            barrier, inc=1, device_id={"sp": lax.rem(sp + k, sp_count)}, device_id_type=MESH
        )
    pl.semaphore_wait(barrier, tp + 1)

    def rows_of(c):
        return pl.ds(pl.multiple_of(c * BLOCK, BLOCK), BLOCK)

    def block_of(kind, l, c, slot):
        return gather.at[kind, l, slot, rows_of(c)]

    def direct(kind, l, c, peer, source):
        ref = block_of(kind, l, c, source)
        return remote(
            ref, ref, g_send.at[kind, c, peer], g_recv.at[kind, l, c, source], {"tp": peer}
        )

    def forward(kind, l, c, source):
        ref = block_of(kind, l, c, source)
        return remote(
            ref, ref, f_send.at[kind, c, source], g_recv.at[kind, l, c, source], {"tp": sibling}
        )

    def spread(kind, l, c):
        for k in range(1, ychips):
            direct(kind, l, c, lax.rem(me + 2 * k, tp), me).start()
        direct(kind, l, c, sibling, me).start()

    def relay(kind, l, c):
        for k in range(1, ychips):
            source = lax.rem(me + 2 * k, tp)
            direct(kind, l, c, source, source).wait_recv()
            forward(kind, l, c, source).start()

    def arrive(kind, l, c):
        direct(kind, l, c, sibling, sibling).wait_recv()
        for k in range(1, ychips):
            source = lax.rem(sibling + 2 * k, tp)
            direct(kind, l, c, sibling, source).wait_recv()
        for k in range(1, ychips):
            forward(kind, l, c, lax.rem(me + 2 * k, tp)).wait_send()
            direct(kind, l, c, lax.rem(me + 2 * k, tp), me).wait_send()
        direct(kind, l, c, sibling, me).wait_send()

    def halo(l, c, which):
        buf = (kbuf, vbuf)[which]
        return remote(
            buf.at[l, rows_of(c + blocks)],
            buf.at[l, rows_of(c)],
            h_send.at[c, which],
            h_recv.at[l, c, which],
            {"sp": lax.rem(sp + 1, sp_count)},
        )

    def sum_copy(l, c, peer, source):
        ref = sums.at[l, c, source]
        return remote(ref, ref, s_send.at[peer], s_recv.at[l, c, source], {"tp": peer})

    gather[0, 0, me] = res_ref[...]
    for t in range(chunks):
        spread(0, 0, chunks - 1 - t)

    @pl.when(sp == 0)
    def _():
        for l in range(layers):
            kbuf[l, :reach] = jnp.zeros((reach, cols), BF16)
            vbuf[l, :reach] = jnp.zeros((reach, cols), BF16)

    row = lax.broadcasted_iota(jnp.int32, (BLOCK, BLOCK), 0)
    col = lax.broadcasted_iota(jnp.int32, (BLOCK, BLOCK), 1)
    low = col < HEAD
    early = jnp.where((row >= SEG) & (col < SEG), NEG, 0.0).astype(F32)
    late = jnp.where((row < SEG) & (col >= SEG), NEG, 0.0).astype(F32)

    def project(l, c):
        arrive(0, l, c)
        parts = [gather[0, l, j, rows_of(c)].astype(F32) for j in range(tp)]
        total = sum(jnp.sum(p * p, axis=1, keepdims=True) for p in parts)
        inv = lax.rsqrt(total / width + EPS)
        gain = gains_ref[l, 0:1, :]
        normed = jnp.concatenate(
            [
                (p * inv * gain[:, j * cols : (j + 1) * cols]).astype(BF16)
                for j, p in enumerate(parts)
            ],
            axis=1,
        )
        own = rows_of(c + blocks)
        kbuf[l, own] = jnp.dot(normed, wbuf[l, 1], preferred_element_type=F32).astype(BF16)
        vbuf[l, own] = jnp.dot(normed, wbuf[l, 2], preferred_element_type=F32).astype(BF16)

        @pl.when(sp < sp_count - 1)
        def _():
            halo(l, c, 0).start()
            halo(l, c, 1).start()

        query = jnp.dot(normed, wbuf[l, 0], preferred_element_type=F32)
        qbuf[rows_of(c)] = (query * (LOG2E * HEAD**-0.5)).astype(BF16)

    def attention(l, c):
        @pl.when(sp > 0)
        def _():
            halo(l, c, 0).wait_recv()
            halo(l, c, 1).wait_recv()

        @pl.when(sp < sp_count - 1)
        def _():
            halo(l, c, 0).wait_send()
            halo(l, c, 1).wait_send()

        window = pl.ds(pl.multiple_of(c * BLOCK, BLOCK), reach + BLOCK)
        closed = [
            jnp.where((sp == 0) & (c + i < blocks), NEG, 0.0).astype(F32) for i in range(blocks)
        ]

        for pair in range(pairs):
            lanes = slice(pair * 128, (pair + 1) * 128)
            query = qbuf[rows_of(c), lanes]
            keys = kbuf[l, window, lanes]
            values = vbuf[l, window, lanes]
            halves = []
            for half in range(2):
                mine = low if half == 0 else ~low
                masked = jnp.where(mine, query.astype(F32), 0.0).astype(BF16)
                scores = lax.dot_general(
                    masked, keys, (((1,), (1,)), ((), ())), preferred_element_type=F32
                )
                tiles = []
                for i in range(blocks + 1):
                    tile = scores[:, i * BLOCK : (i + 1) * BLOCK]
                    if i == 0:
                        tile = tile + early
                    if i >= blocks - 1:
                        at = (i - blocks + 1) * BLOCK
                        tile = tile + toeplitz[l, 2 * pair + half, :, at : at + BLOCK]
                    if i < blocks:
                        tile = tile + closed[i]
                    tiles.append(tile)
                top = functools.reduce(jnp.maximum, tiles)
                top = jnp.max(top, axis=1, keepdims=True)
                tiles = [jnp.exp2(tile - top) for tile in tiles]
                total = jnp.sum(functools.reduce(jnp.add, tiles), axis=1, keepdims=True)
                raw = jnp.concatenate([tile.astype(BF16) for tile in tiles], axis=1)
                mixed = jnp.dot(raw, values, preferred_element_type=F32)
                halves.append(mixed / total)
            gather[1, l, me, rows_of(c), lanes] = jnp.where(low, halves[0], halves[1]).astype(BF16)
        spread(1, l, c)

    def out_project(l, c):
        arrive(1, l, c)
        whole = jnp.concatenate([gather[1, l, j, rows_of(c)] for j in range(tp)], axis=1)
        value = jnp.dot(whole, wbuf[l, 3], preferred_element_type=F32)
        branch[rows_of(c)] = value
        square = jnp.sum(value * value, axis=1, keepdims=True)
        sums[l, c, me] = jnp.broadcast_to(square, (BLOCK, BLOCK)).T[:8]
        for k in range(1, tp):
            sum_copy(l, c, lax.rem(me + k, tp), me).start()

    def finish(l, c):
        for k in range(1, tp):
            peer = lax.rem(me + k, tp)
            sum_copy(l, c, peer, peer).wait_recv()
            sum_copy(l, c, peer, me).wait_send()
        total = functools.reduce(jnp.add, [sums[l, c, j] for j in range(tp)])
        inv = lax.rsqrt(total / width + EPS)
        inv = jnp.broadcast_to(inv[0:1], (BLOCK, BLOCK)).T[:, 0:1]
        gain = gains_ref[l, 1:2, pl.ds(pl.multiple_of(me * cols, 128), cols)]
        new = gather[0, l, me, rows_of(c)].astype(F32) + branch[rows_of(c)] * inv * gain
        new = new.astype(BF16)

        @pl.when(l == layers - 1)
        def _():
            out_ref[rows_of(c)] = new

        @pl.when(l < layers - 1)
        def _():
            later = jnp.minimum(l + 1, layers - 1)
            gather[0, later, me, rows_of(c)] = new
            spread(0, later, c)

    def tables(l, carry):
        far = bias_ref[l, :, 2 * MAXREL :]
        near = (bias_ref[l, :, : 2 * MAXREL] - far) * LOG2E
        for h in range(2 * pairs):
            line = jnp.concatenate([jnp.zeros((1, BLOCK), F32), near[h : h + 1]], axis=1)
            line = jnp.broadcast_to(line, (2 * BLOCK, 3 * BLOCK))
            skewed = pltpu.roll(line, 0, 1, stride=1, stride_axis=0)
            toeplitz[l, h, :, :BLOCK] = skewed[:BLOCK, :BLOCK].T
            toeplitz[l, h, :, BLOCK:] = skewed[BLOCK:, :BLOCK].T + late
        return carry

    lax.fori_loop(0, layers, tables, 0)

    for k in range(3):
        weight_copy(0, k).wait()

    def enter(t, carry):
        @pl.when(t < chunks)
        def _():
            relay(0, 0, chunks - 1 - t)

        @pl.when(t >= 1)
        def _():
            project(0, chunks - t)

        return carry

    lax.fori_loop(0, chunks + 1, enter, 0)
    weight_copy(0, 3).wait()

    def layer(l, carry):
        later = jnp.minimum(l + 1, layers - 1)
        more = l < layers - 1

        def stage(t, lag, needed=True):
            return (t >= lag) & (t < lag + chunks) & needed

        def step(t, carry):
            def at(lag):
                return chunks - 1 - t + lag

            @pl.when(stage(t, 0))
            def _():
                attention(l, at(0))

            @pl.when(stage(t, 1))
            def _():
                relay(1, l, at(1))

            @pl.when(stage(t, 2))
            def _():
                out_project(l, at(2))

            @pl.when(stage(t, 3))
            def _():
                finish(l, at(3))

            @pl.when((t == 4) & more)
            def _():
                for k in range(4):
                    weight_copy(later, k).wait()

            @pl.when(stage(t, 4, more))
            def _():
                relay(0, later, at(4))

            @pl.when(stage(t, 5, more))
            def _():
                project(later, at(5))

            return carry

        lax.fori_loop(0, chunks + 5, step, 0)
        return carry

    lax.fori_loop(0, layers, layer, 0)


def on_device(tp, sp_count, residual, gains, w_query, w_key, w_value, w_out, rel_bias):
    tokens, cols = residual.shape
    layers, width, _ = w_query.shape
    chunks = tokens // BLOCK
    reach = LEFT * SEG
    heads = cols // HEAD
    vmem = pl.BlockSpec(memory_space=pltpu.VMEM)
    hbm = pl.BlockSpec(memory_space=pl.ANY)
    dma = pltpu.SemaphoreType.DMA
    return pl.pallas_call(
        functools.partial(kernel, tp, sp_count),
        out_shape=jax.ShapeDtypeStruct((tokens, cols), BF16),
        in_specs=[vmem, vmem, vmem, hbm, hbm, hbm, hbm],
        out_specs=vmem,
        scratch_shapes=[
            pltpu.VMEM((layers, 4, width, cols), BF16),
            pltpu.VMEM((2, layers, tp, tokens, cols), BF16),
            pltpu.VMEM((layers, reach + tokens, cols), BF16),
            pltpu.VMEM((layers, reach + tokens, cols), BF16),
            pltpu.VMEM((tokens, cols), BF16),
            pltpu.VMEM((tokens, cols), F32),
            pltpu.VMEM((layers, heads, BLOCK, 2 * BLOCK), F32),
            pltpu.VMEM((layers, chunks, tp, 8, BLOCK), F32),
            dma((layers, 4)),
            dma((2, chunks, tp)),
            dma((2, layers, chunks, tp)),
            dma((2, chunks, tp)),
            dma((chunks, 2)),
            dma((layers, chunks, 2)),
            dma((tp,)),
            dma((layers, chunks, tp)),
        ],
        compiler_params=pltpu.CompilerParams(
            collective_id=0, has_side_effects=True, vmem_limit_bytes=58 * 2**20
        ),
    )(residual, gains, rel_bias, w_query, w_key, w_value, w_out)


def solution(mesh):
    return jax.shard_map(
        functools.partial(on_device, mesh.shape["tp"], mesh.shape["sp"]),
        mesh=mesh,
        in_specs=(
            P("sp", "tp"),
            P(),
            P(None, None, "tp"),
            P(None, None, "tp"),
            P(None, None, "tp"),
            P(None, None, "tp"),
            P(None, "tp", None),
        ),
        out_specs=P("sp", "tp"),
        check_vma=False,
    )
```

```python
import functools

import jax
import jax.numpy as jnp
from jax import lax
from jax.experimental import pallas as pl
from jax.experimental.pallas import tpu as pltpu
from jax.sharding import PartitionSpec as P

HEAD = 64
SEG = 64
LEFT = 8
MAXREL = 128
BLOCK = 128
EPS = 1e-06
LOG2E = 1.4426950408889634
NEG = -1e30
MESH = pl.DeviceIdType.MESH
F32 = jnp.float32
BF16 = jnp.bfloat16


def remote(src, dst, send_sem, recv_sem, where):
    return pltpu.make_async_remote_copy(
        src_ref=src,
        dst_ref=dst,
        send_sem=send_sem,
        recv_sem=recv_sem,
        device_id=where,
        device_id_type=MESH,
    )


def kernel(
    tp,
    sp_count,
    res_ref,
    gains_ref,
    bias_ref,
    wq_ref,
    wk_ref,
    wv_ref,
    wo_ref,
    out_ref,
    wbuf,
    gather,
    kbuf,
    vbuf,
    qbuf,
    branch,
    toeplitz,
    sums,
    w_sem,
    g_send,
    g_recv,
    f_send,
    h_send,
    h_recv,
    s_send,
    s_recv,
):
    layers = wbuf.shape[0]
    tokens, cols = res_ref.shape
    width = cols * tp
    chunks = tokens // BLOCK
    pairs = cols // 128
    reach = LEFT * SEG
    blocks = reach // BLOCK
    me = lax.axis_index("tp")
    sp = lax.axis_index("sp")
    core = lax.rem(me, 2)
    sibling = me + 1 - 2 * core
    ychips = tp // 2

    weights = (wq_ref, wk_ref, wv_ref, wo_ref)

    def weight_copy(l, k):
        return pltpu.make_async_copy(weights[k].at[l], wbuf.at[l, k], w_sem.at[l, k])

    for l in range(layers):
        for k in range(4):
            weight_copy(l, k).start()

    barrier = pltpu.get_barrier_semaphore()
    for k in range(1, tp):
        pl.semaphore_signal(
            barrier, inc=1, device_id={"tp": lax.rem(me + k, tp)}, device_id_type=MESH
        )
    for k in (1, sp_count - 1):
        pl.semaphore_signal(
            barrier, inc=1, device_id={"sp": lax.rem(sp + k, sp_count)}, device_id_type=MESH
        )
    pl.semaphore_wait(barrier, tp + 1)

    def rows_of(c):
        return pl.ds(pl.multiple_of(c * BLOCK, BLOCK), BLOCK)

    def block_of(kind, l, c, slot):
        return gather.at[kind, l, slot, rows_of(c)]

    def direct(kind, l, c, peer, source):
        ref = block_of(kind, l, c, source)
        return remote(
            ref, ref, g_send.at[kind, c, peer], g_recv.at[kind, l, c, source], {"tp": peer}
        )

    def forward(kind, l, c, source):
        ref = block_of(kind, l, c, source)
        return remote(
            ref, ref, f_send.at[kind, c, source], g_recv.at[kind, l, c, source], {"tp": sibling}
        )

    def spread(kind, l, c):
        for k in range(1, ychips):
            direct(kind, l, c, lax.rem(me + 2 * k, tp), me).start()
        direct(kind, l, c, sibling, me).start()

    def relay(kind, l, c):
        for k in range(1, ychips):
            source = lax.rem(me + 2 * k, tp)
            direct(kind, l, c, source, source).wait_recv()
            forward(kind, l, c, source).start()

    def arrive(kind, l, c):
        direct(kind, l, c, sibling, sibling).wait_recv()
        for k in range(1, ychips):
            source = lax.rem(sibling + 2 * k, tp)
            direct(kind, l, c, sibling, source).wait_recv()
        for k in range(1, ychips):
            forward(kind, l, c, lax.rem(me + 2 * k, tp)).wait_send()
            direct(kind, l, c, lax.rem(me + 2 * k, tp), me).wait_send()
        direct(kind, l, c, sibling, me).wait_send()

    def halo(l, c, which):
        buf = (kbuf, vbuf)[which]
        return remote(
            buf.at[l, rows_of(c + blocks)],
            buf.at[l, rows_of(c)],
            h_send.at[c, which],
            h_recv.at[l, c, which],
            {"sp": lax.rem(sp + 1, sp_count)},
        )

    def sum_copy(l, c, peer, source):
        ref = sums.at[l, c, source]
        return remote(ref, ref, s_send.at[peer], s_recv.at[l, c, source], {"tp": peer})

    gather[0, 0, me] = res_ref[...]
    for t in range(chunks):
        spread(0, 0, chunks - 1 - t)

    @pl.when(sp == 0)
    def _():
        for l in range(layers):
            kbuf[l, :reach] = jnp.zeros((reach, cols), BF16)
            vbuf[l, :reach] = jnp.zeros((reach, cols), BF16)

    row = lax.broadcasted_iota(jnp.int32, (BLOCK, BLOCK), 0)
    col = lax.broadcasted_iota(jnp.int32, (BLOCK, BLOCK), 1)
    low = col < HEAD
    early = jnp.where((row >= SEG) & (col < SEG), NEG, 0.0).astype(F32)
    late = jnp.where((row < SEG) & (col >= SEG), NEG, 0.0).astype(F32)

    def project(l, c):
        arrive(0, l, c)
        parts = [gather[0, l, j, rows_of(c)].astype(F32) for j in range(tp)]
        total = sum(jnp.sum(p * p, axis=1, keepdims=True) for p in parts)
        inv = lax.rsqrt(total / width + EPS)
        gain = gains_ref[l, 0:1, :]
        normed = jnp.concatenate(
            [
                (p * inv * gain[:, j * cols : (j + 1) * cols]).astype(BF16)
                for j, p in enumerate(parts)
            ],
            axis=1,
        )
        own = rows_of(c + blocks)
        kbuf[l, own] = jnp.dot(normed, wbuf[l, 1], preferred_element_type=F32).astype(BF16)
        vbuf[l, own] = jnp.dot(normed, wbuf[l, 2], preferred_element_type=F32).astype(BF16)

        @pl.when(sp < sp_count - 1)
        def _():
            halo(l, c, 0).start()
            halo(l, c, 1).start()

        query = jnp.dot(normed, wbuf[l, 0], preferred_element_type=F32)
        qbuf[rows_of(c)] = (query * (LOG2E * HEAD**-0.5)).astype(BF16)

    def attention(l, c):
        @pl.when(sp > 0)
        def _():
            halo(l, c, 0).wait_recv()
            halo(l, c, 1).wait_recv()

        @pl.when(sp < sp_count - 1)
        def _():
            halo(l, c, 0).wait_send()
            halo(l, c, 1).wait_send()

        window = pl.ds(pl.multiple_of(c * BLOCK, BLOCK), reach + BLOCK)
        closed = [
            jnp.where((sp == 0) & (c + i < blocks), NEG, 0.0).astype(F32) for i in range(blocks)
        ]

        for pair in range(pairs):
            if pair == pairs // 2:

                @pl.when(c < chunks - 1)
                def _():
                    relay(1, l, jnp.minimum(c + 1, chunks - 1))

            lanes = slice(pair * 128, (pair + 1) * 128)
            query = qbuf[rows_of(c), lanes]
            keys = kbuf[l, window, lanes]
            values = vbuf[l, window, lanes]
            halves = []
            for half in range(2):
                mine = low if half == 0 else ~low
                masked = jnp.where(mine, query.astype(F32), 0.0).astype(BF16)
                scores = lax.dot_general(
                    masked, keys, (((1,), (1,)), ((), ())), preferred_element_type=F32
                )
                tiles = []
                for i in range(blocks + 1):
                    tile = scores[:, i * BLOCK : (i + 1) * BLOCK]
                    if i == 0:
                        tile = tile + early
                    if i >= blocks - 1:
                        at = (i - blocks + 1) * BLOCK
                        tile = tile + toeplitz[l, 2 * pair + half, :, at : at + BLOCK]
                    if i < blocks:
                        tile = tile + closed[i]
                    tiles.append(tile)
                top = functools.reduce(jnp.maximum, tiles)
                top = jnp.max(top, axis=1, keepdims=True)
                tiles = [jnp.exp2(tile - top) for tile in tiles]
                total = jnp.sum(functools.reduce(jnp.add, tiles), axis=1, keepdims=True)
                raw = jnp.concatenate([tile.astype(BF16) for tile in tiles], axis=1)
                mixed = jnp.dot(raw, values, preferred_element_type=F32)
                halves.append(mixed / total)
            gather[1, l, me, rows_of(c), lanes] = jnp.where(low, halves[0], halves[1]).astype(BF16)
        spread(1, l, c)

    def out_project(l, c):
        arrive(1, l, c)
        whole = jnp.concatenate([gather[1, l, j, rows_of(c)] for j in range(tp)], axis=1)
        value = jnp.dot(whole, wbuf[l, 3], preferred_element_type=F32)
        branch[rows_of(c)] = value
        square = jnp.sum(value * value, axis=1, keepdims=True)
        sums[l, c, me] = jnp.broadcast_to(square, (BLOCK, BLOCK)).T[:8]
        for k in range(1, tp):
            sum_copy(l, c, lax.rem(me + k, tp), me).start()

    def finish(l, c):
        for k in range(1, tp):
            peer = lax.rem(me + k, tp)
            sum_copy(l, c, peer, peer).wait_recv()
            sum_copy(l, c, peer, me).wait_send()
        total = functools.reduce(jnp.add, [sums[l, c, j] for j in range(tp)])
        inv = lax.rsqrt(total / width + EPS)
        inv = jnp.broadcast_to(inv[0:1], (BLOCK, BLOCK)).T[:, 0:1]
        gain = gains_ref[l, 1:2, pl.ds(pl.multiple_of(me * cols, 128), cols)]
        new = gather[0, l, me, rows_of(c)].astype(F32) + branch[rows_of(c)] * inv * gain
        new = new.astype(BF16)

        @pl.when(l == layers - 1)
        def _():
            out_ref[rows_of(c)] = new

        @pl.when(l < layers - 1)
        def _():
            later = jnp.minimum(l + 1, layers - 1)
            gather[0, later, me, rows_of(c)] = new
            spread(0, later, c)

    def tables(l, carry):
        far = bias_ref[l, :, 2 * MAXREL :]
        near = (bias_ref[l, :, : 2 * MAXREL] - far) * LOG2E
        for h in range(2 * pairs):
            line = jnp.concatenate([jnp.zeros((1, BLOCK), F32), near[h : h + 1]], axis=1)
            line = jnp.broadcast_to(line, (2 * BLOCK, 3 * BLOCK))
            skewed = pltpu.roll(line, 0, 1, stride=1, stride_axis=0)
            toeplitz[l, h, :, :BLOCK] = skewed[:BLOCK, :BLOCK].T
            toeplitz[l, h, :, BLOCK:] = skewed[BLOCK:, :BLOCK].T + late
        return carry

    lax.fori_loop(0, layers, tables, 0)

    for k in range(3):
        weight_copy(0, k).wait()

    def enter(t, carry):
        @pl.when(t < chunks)
        def _():
            relay(0, 0, chunks - 1 - t)

        @pl.when(t >= 1)
        def _():
            project(0, chunks - t)

        return carry

    lax.fori_loop(0, chunks + 1, enter, 0)
    weight_copy(0, 3).wait()

    def layer(l, carry):
        later = jnp.minimum(l + 1, layers - 1)
        more = l < layers - 1

        def stage(t, lag, needed=True):
            return (t >= lag) & (t < lag + chunks) & needed

        def step(t, carry):
            def at(lag):
                return chunks - 1 - t + lag

            @pl.when(stage(t, 0))
            def _():
                attention(l, at(0))

            @pl.when(t == chunks)
            def _():
                relay(1, l, 0)

            @pl.when(stage(t, 1))
            def _():
                out_project(l, at(1))

            @pl.when(stage(t, 2))
            def _():
                finish(l, at(2))

            @pl.when((t == 3) & more)
            def _():
                for k in range(4):
                    weight_copy(later, k).wait()

            @pl.when(stage(t, 3, more))
            def _():
                relay(0, later, at(3))

            @pl.when(stage(t, 4, more))
            def _():
                project(later, at(4))

            return carry

        lax.fori_loop(0, chunks + 4, step, 0)
        return carry

    lax.fori_loop(0, layers, layer, 0)


def on_device(tp, sp_count, residual, gains, w_query, w_key, w_value, w_out, rel_bias):
    tokens, cols = residual.shape
    layers, width, _ = w_query.shape
    chunks = tokens // BLOCK
    reach = LEFT * SEG
    heads = cols // HEAD
    vmem = pl.BlockSpec(memory_space=pltpu.VMEM)
    hbm = pl.BlockSpec(memory_space=pl.ANY)
    dma = pltpu.SemaphoreType.DMA
    return pl.pallas_call(
        functools.partial(kernel, tp, sp_count),
        out_shape=jax.ShapeDtypeStruct((tokens, cols), BF16),
        in_specs=[vmem, vmem, vmem, hbm, hbm, hbm, hbm],
        out_specs=vmem,
        scratch_shapes=[
            pltpu.VMEM((layers, 4, width, cols), BF16),
            pltpu.VMEM((2, layers, tp, tokens, cols), BF16),
            pltpu.VMEM((layers, reach + tokens, cols), BF16),
            pltpu.VMEM((layers, reach + tokens, cols), BF16),
            pltpu.VMEM((tokens, cols), BF16),
            pltpu.VMEM((tokens, cols), F32),
            pltpu.VMEM((layers, heads, BLOCK, 2 * BLOCK), F32),
            pltpu.VMEM((layers, chunks, tp, 8, BLOCK), F32),
            dma((layers, 4)),
            dma((2, chunks, tp)),
            dma((2, layers, chunks, tp)),
            dma((2, chunks, tp)),
            dma((chunks, 2)),
            dma((layers, chunks, 2)),
            dma((tp,)),
            dma((layers, chunks, tp)),
        ],
        compiler_params=pltpu.CompilerParams(
            collective_id=0, has_side_effects=True, vmem_limit_bytes=58 * 2**20
        ),
    )(residual, gains, rel_bias, w_query, w_key, w_value, w_out)


def solution(mesh):
    return jax.shard_map(
        functools.partial(on_device, mesh.shape["tp"], mesh.shape["sp"]),
        mesh=mesh,
        in_specs=(
            P("sp", "tp"),
            P(),
            P(None, None, "tp"),
            P(None, None, "tp"),
            P(None, None, "tp"),
            P(None, None, "tp"),
            P(None, "tp", None),
        ),
        out_specs=P("sp", "tp"),
        check_vma=False,
    )
```
